32 devices in a mesh: ep: 8 (over z, x), tp: 4 (over y, core).
Axes of the slice: x: 2, y: 2, z: 4, core: 2. Of those that a mesh axis runs over, the one named last changes fastest.
Arguments:
- recurrence_query: bfloat16 [1024, 1024], P('ep', 'tp'), may hold values from -6 to 6
- forget_preactivation: bfloat16 [1024, 1024], P('ep', 'tp'), may hold values from -7 to 7
- recurrence_value: bfloat16 [1024, 1024], P('ep', 'tp'), may hold values from -6 to 6
- output_gate_preactivation: bfloat16 [1024, 1024], P('ep', 'tp'), may hold values from -6 to 6
- forget_margin: float32 [1024], P('tp'), may hold values from 0 to 0.1
- surge_log_decay: float32 [8, 1024], P('tp', 'ep'), may hold values from -1.4 to 0
- head_norm_gain: float32 [1024], P('tp'), may hold values from 0.1 to 1.9
- recurrence_output_matrix: bfloat16 [1024, 4096], P('tp'), may hold values from -0.1875 to 0.1875
- second_micro_input: bfloat16 [1024, 4096], P(('ep', 'tp')), may hold values from -6 to 6
- expert_norm_gain: float32 [4096], replicated, may hold values from 0.1 to 1.9
- routes: int32 [1024, 2], P('ep'), may hold values from 0 to 7, all different within a row; in each aligned block of 32 rows (0 to 31, 32 to 63, ...) at most 16 rows name the same one
- router_chosen_logits: float32 [1024, 2], P(('ep', 'tp')), may hold values from -6 to 6
- expert_gate_matrix: bfloat16 [8, 4096, 1408], P('ep', None, 'tp'), may hold values from -0.09375 to 0.09375
- expert_up_matrix: bfloat16 [8, 4096, 1408], P('ep', None, 'tp'), may hold values from -0.09375 to 0.09375
- expert_down_matrix: bfloat16 [8, 1408, 4096], P('ep', 'tp'), may hold values from -0.15625 to 0.15625
Outputs:
- mixed: bfloat16 [1024, 4096], P(('ep', 'tp'))
- moe_out: bfloat16 [1024, 4096], P(('ep', 'tp'))
The draws below stay inside these ranges and needn't reach their ends.
Inputs may be any that keep to these rules, and one draw needn't show every extreme that they name: `routes`: in the rows of one device (aligned blocks of 32 rows) no expert is named more than 16 times, and the experts of a row differ.
All inputs are finite; a program needn't handle non-finite values.
Results may differ from the reference program's by a relative error of at most 0.019.
Values may be sent and summed in bfloat16 or wider, within the bound.
A program may use at most 128 MiB of HBM per device.

```python
import math
import jax
import jax.numpy as jnp
import numpy as np
from jax import lax

D = 4096
HEADS = 8
KEY = 128
VAL = 128
FF = 1408
TOP = 2
SPAN = 64
SEQ_DEV = 128
TB_DEV = 32
EXPERTS = 8
CAP = 16
TOKENS_A = 1024
TOKENS_B = 1024
N_EP = 8
N_TP = 4


def draw_forget_preactivation(key, part):
    noise_key, shift_key = jax.random.split(jax.random.fold_in(key, 11))
    blocks = TOKENS_A // SEQ_DEV
    shifts = jax.random.uniform(shift_key, (blocks, 1, HEADS * KEY), jnp.float32, -1.0, 1.0)
    noise = jnp.clip(jax.random.normal(noise_key, (blocks, SEQ_DEV, HEADS * KEY), jnp.float32), -6.0, 6.0)
    return (noise + shifts).reshape(TOKENS_A, HEADS * KEY).astype(jnp.bfloat16)


def draw_forget_margin(key, part):
    pick_key, fast_key, slow_key = jax.random.split(jax.random.fold_in(key, 23), 3)
    share = 0.5
    fast_head = jax.random.uniform(pick_key, (HEADS, 1), jnp.float32) < share
    fast_gap = jnp.exp(jax.random.uniform(fast_key, (HEADS, KEY), jnp.float32, math.log(0.04), math.log(0.1)))
    slow_gap = jnp.exp(jax.random.uniform(slow_key, (HEADS, KEY), jnp.float32, math.log(0.3), math.log(1.5))) / TOKENS_A
    return jnp.where(fast_head, fast_gap, slow_gap).reshape(HEADS * KEY).astype(jnp.float32)


def draw_surge_log_decay(key, part):
    spot_key, depth_key = jax.random.split(jax.random.fold_in(key, 37))
    spots = jax.random.randint(spot_key, (HEADS, 2, 1), 0, TOKENS_A)
    depth = jax.random.uniform(depth_key, (HEADS, 2, 1), jnp.float32, math.log(0.5), math.log(0.8))
    hits = spots == jnp.arange(TOKENS_A, dtype=jnp.int32)[None, None, :]
    return jnp.sum(jnp.where(hits, depth, 0.0), axis=1).astype(jnp.float32)


def block_levels(stream_key, extent, shards, low, high):
    level, own = 1.0, jax.random.fold_in(stream_key, 6)
    for axis_at, parts in shards:
        heights = jnp.exp(jax.random.uniform(jax.random.fold_in(own, axis_at), (parts,), jnp.float32, low / len(shards), high / len(shards)))
        level = level * jnp.repeat(heights, extent[axis_at] // parts).reshape([-1 if axis == axis_at else 1 for axis in range(len(extent))])
    return level


def deal_out(own_key, own, number, rows, amount, top, most, slope):
    order = jax.random.permutation(own_key, amount)
    heavy_load, ordinary = shares(amount, rows * top, most, slope, True), shares(amount, rows * top, most, slope, False)
    places = jnp.arange(amount)

    def named(tallies, turn):
        used = int((tallies > 0).sum())
        fixed = max(1, used // 4)
        passed = fixed + (places - fixed + turn * (used - fixed)) % max(1, amount - fixed)
        return jnp.zeros((amount,), jnp.int32).at[order[jnp.where(places < fixed, places, passed)]].set(jnp.asarray(tallies, jnp.int32))

    tallies = jnp.where(number % 4 == 0, named(heavy_load, number // 4), named(ordinary, number - number // 4 - 1))
    mixed = jax.random.permutation(jax.random.fold_in(own, 3), amount)
    donor, taker = mixed[0:amount // 2 * 2:2], mixed[1:amount // 2 * 2:2]
    margin = jnp.minimum(tallies[donor] - 1, most - tallies[taker]) // 2
    margin = jnp.where((donor == order[0]) | (taker == order[0]) | (tallies[taker] == 0), 0, jnp.maximum(margin, 0))
    passed = jax.random.randint(jax.random.fold_in(own, 4), (amount // 2,), 0, 1 << 20) % (margin + 1)
    tallies = tallies.at[donor].add(-passed).at[taker].add(passed)
    items = jnp.searchsorted(jnp.cumsum(tallies), jnp.arange(rows * top), side="right").astype(jnp.int32)
    grid = items.reshape(top, rows).T
    grid = grid[jax.random.permutation(jax.random.fold_in(own, 1), rows)]
    turn = jax.random.randint(jax.random.fold_in(own, 2), (rows, 1), 0, top)
    return jnp.take_along_axis(grid, (jnp.arange(top)[None, :] + turn) % top, axis=1)


def shares(count, total, bound, slope, full):
    weights = [(1 << 20) // math.isqrt(grade ** slope) + 1 for grade in range(1, count + 1)]
    largest = bound if full else min(bound, max(-(-total // count), total * weights[0] // sum(weights)))
    least = 1 if total - largest >= count - 1 else 0
    holding, surplus = [largest] + [least] * (count - 1), total - largest - least * (count - 1)
    while surplus > 0:
        candidates = [i for i in range(1, count) if holding[i] < largest] or [i for i in range(1, count) if holding[i] < bound]
        whole, remaining = sum([weights[i] for i in candidates]), surplus
        for i in candidates:
            addition = min(bound - holding[i], max(1, remaining * weights[i] // whole), surplus)
            holding[i] = holding[i] + addition
            surplus = surplus - addition
    return np.array(holding)


def normal_values(rng, dims, deviation, reach, shards=(), kind=jnp.bfloat16):
    values = jax.random.normal(rng, dims, jnp.float32) * deviation
    if len(shards) > 0:
        values = block_levels(rng, dims, shards, -0.22, 0.18) * values
    return jnp.clip(values, min=-reach, max=reach).astype(kind)


def setup_inputs(seed: int = 0) -> dict:
    streams_of = jax.random.split(jax.random.key(seed), 16)
    recurrence_query = normal_values(streams_of[0], (TOKENS_A, HEADS * KEY), 1.0, 6.0, ((0, 8), (1, 4)))
    forget_preactivation = draw_forget_preactivation(jax.random.fold_in(streams_of[15], 71), 0)
    recurrence_value = normal_values(streams_of[2], (TOKENS_A, HEADS * VAL), 1.0, 6.0, ((0, 8), (1, 4)))
    output_gate_preactivation = normal_values(streams_of[3], (TOKENS_A, HEADS * VAL), 1.0, 6.0, ((0, 8), (1, 4)))
    forget_margin = draw_forget_margin(jax.random.fold_in(streams_of[15], 71), 0)
    surge_log_decay = draw_surge_log_decay(jax.random.fold_in(streams_of[15], 71), 0)
    head_norm_gain = jnp.clip(1.0 + 0.18 * jax.random.normal(streams_of[6], (HEADS * VAL,), jnp.float32), 0.1, 1.9)
    recurrence_output_matrix = normal_values(streams_of[7], (HEADS * VAL, D), (HEADS * VAL) ** -0.5, 0.1875, ((0, 4),))
    second_micro_input = normal_values(streams_of[8], (TOKENS_B, D), 1.0, 6.0, ((0, 32),))
    expert_norm_gain = jnp.clip(1.0 + 0.18 * jax.random.normal(streams_of[9], (D,), jnp.float32), 0.1, 1.9)
    routes_keys = jax.random.split(jax.random.fold_in(streams_of[10], 1), TOKENS_B // TB_DEV)
    routes_turns = jax.random.permutation(jax.random.fold_in(streams_of[10], 3), TOKENS_B // TB_DEV)
    routes = jax.vmap(lambda own, number: deal_out(jax.random.fold_in(streams_of[10], 2), own, number, TB_DEV, EXPERTS, TOP, CAP, 1))(routes_keys, routes_turns).reshape((TOKENS_B, TOP))
    router_chosen_logits = normal_values(streams_of[11], (TOKENS_B, TOP), 1.0, 6.0, ((0, 32),), jnp.float32)
    expert_gate_matrix = normal_values(streams_of[12], (EXPERTS, D, FF), D ** -0.5, 0.09375, ((0, 8), (2, 4)))
    expert_up_matrix = normal_values(streams_of[13], (EXPERTS, D, FF), D ** -0.5, 0.09375, ((0, 8), (2, 4)))
    expert_down_matrix = normal_values(streams_of[14], (EXPERTS, FF, D), FF ** -0.5, 0.15625, ((0, 8), (1, 4)))
    return {"recurrence_query": recurrence_query, "forget_preactivation": forget_preactivation, "recurrence_value": recurrence_value, "output_gate_preactivation": output_gate_preactivation, "forget_margin": forget_margin, "surge_log_decay": surge_log_decay, "head_norm_gain": head_norm_gain, "recurrence_output_matrix": recurrence_output_matrix, "second_micro_input": second_micro_input, "expert_norm_gain": expert_norm_gain, "routes": routes, "router_chosen_logits": router_chosen_logits, "expert_gate_matrix": expert_gate_matrix, "expert_up_matrix": expert_up_matrix, "expert_down_matrix": expert_down_matrix}


epsilon = 1e-06
highest = lax.Precision.HIGHEST

def span_recurrence(query, inflow, decay_logarithm, values):
    number_of_heads, seq_len, key_width = query.shape
    span_count = seq_len // SPAN

    def to_spans(array):
        return array.reshape(number_of_heads, span_count, SPAN, array.shape[-1]).transpose(1, 0, 2, 3)
    lower_mask = jnp.tril(jnp.ones((SPAN, SPAN), bool))

    def advance(carried, inputs):
        query_span, inflow_span, decay_span, value_span = inputs
        running = jnp.cumsum(decay_span, axis=1)
        lifted_query = query_span * jnp.exp(running)
        lowered_inflow = inflow_span * jnp.exp(-running)
        scores = jnp.einsum('htd,hsd->hts', lifted_query, lowered_inflow, precision=highest)
        scores = jnp.where(lower_mask[None, :, :], scores, 0.0)
        output = jnp.einsum('hts,hsv->htv', scores, value_span, precision=highest)
        output = output + jnp.einsum('htd,hdv->htv', lifted_query, carried, precision=highest)
        closing = running[:, -1:, :]
        updated = jnp.exp(closing[:, 0, :])[:, :, None] * carried + jnp.einsum('hsd,hsv->hdv', inflow_span * jnp.exp(closing - running), value_span, precision=highest)
        return (updated, output)
    start_state = jnp.zeros((number_of_heads, key_width, values.shape[-1]), jnp.float32)
    final_state, outputs = lax.scan(advance, start_state, (to_spans(query), to_spans(inflow), to_spans(decay_logarithm), to_spans(values)))
    return (final_state, outputs.transpose(1, 0, 2, 3).reshape(number_of_heads, seq_len, values.shape[-1]))

def split_sum(left, right, groups):
    group_width = left.shape[1] // groups
    total = jnp.zeros((left.shape[0], right.shape[1]), jnp.float32)
    for portion in range(groups):
        piece = jnp.dot(left[:, portion * group_width:(portion + 1) * group_width], right[portion * group_width:(portion + 1) * group_width], preferred_element_type=jnp.float32)
        rounded = lax.optimization_barrier(piece.astype(jnp.bfloat16))
        total = total + rounded.astype(jnp.float32)
    return total.astype(jnp.bfloat16)

def reference(recurrence_query, forget_preactivation, recurrence_value, output_gate_preactivation, forget_margin, surge_log_decay, head_norm_gain, recurrence_output_matrix, second_micro_input, expert_norm_gain, routes, router_chosen_logits, expert_gate_matrix, expert_up_matrix, expert_down_matrix):
    seq_len = recurrence_query.shape[0]

    def heads_leading(array):
        return array.astype(jnp.float32).reshape(seq_len, HEADS, -1).transpose(1, 0, 2)
    closed_flag = jax.nn.sigmoid(-forget_preactivation.astype(jnp.float32)) * forget_margin
    decay_logarithm = heads_leading(jnp.log1p(-closed_flag)) + surge_log_decay[:, :, None]
    query = heads_leading(recurrence_query)
    _, output = span_recurrence(query, heads_leading(closed_flag), decay_logarithm, heads_leading(recurrence_value))
    output = output * lax.rsqrt(lax.optimization_barrier(jnp.mean(output * output, axis=-1, keepdims=True)) + epsilon)
    output = output.transpose(1, 0, 2).reshape(seq_len, -1)
    hidden_a = (output * head_norm_gain * jax.nn.silu(output_gate_preactivation.astype(jnp.float32))).astype(jnp.bfloat16)
    mixed = split_sum(hidden_a, recurrence_output_matrix, N_TP)
    moe_rows = second_micro_input.astype(jnp.float32)
    normed = (moe_rows * lax.rsqrt(lax.optimization_barrier(jnp.mean(moe_rows * moe_rows, axis=-1, keepdims=True)) + epsilon) * expert_norm_gain).astype(jnp.bfloat16)
    flat_routes = routes.reshape(-1)
    copies = flat_routes.shape[0]
    max_rows = N_EP * N_TP * CAP

    def per_expert(written, expert_id):
        picked_order = jnp.argsort((flat_routes != expert_id).astype(jnp.int32), stable=True)[:max_rows]
        picked_order = picked_order.astype(jnp.int32)
        is_live = flat_routes[picked_order] == expert_id
        picked = normed[picked_order // TOP]
        gate_proj = jnp.dot(picked, expert_gate_matrix[expert_id], preferred_element_type=jnp.float32)
        up_proj = jnp.dot(picked, expert_up_matrix[expert_id], preferred_element_type=jnp.float32)
        hidden_b = (jax.nn.silu(gate_proj) * up_proj).astype(jnp.bfloat16)
        result = split_sum(hidden_b, expert_down_matrix[expert_id], N_TP)
        kept_rows = jnp.where(is_live[:, None], result, written[picked_order])
        return (written.at[picked_order].set(kept_rows), None)
    outputs, _ = lax.scan(per_expert, jnp.zeros((copies, D), jnp.bfloat16), jnp.arange(EXPERTS, dtype=jnp.int32))
    route_weight = jax.nn.softmax(router_chosen_logits.astype(jnp.float32), axis=-1)
    moe_out = lax.optimization_barrier(jnp.sum(route_weight[:, :, None] * outputs.reshape(-1, TOP, D).astype(jnp.float32), axis=1))
    return (mixed, moe_out.astype(jnp.bfloat16))
```

```python
import functools

import jax
import jax.numpy as jnp
from jax import lax
from jax.experimental import pallas as pl
from jax.experimental.pallas import tpu as pltpu
from jax.sharding import PartitionSpec as P

TOP = 2
SPAN = 64
MESH = pl.DeviceIdType.MESH


epsilon = 1e-06
wide = jnp.float32
kind = jnp.bfloat16


def visiting_order(count):
    half = count // 2
    near = [(i / max(1, half - 1), i + 1) for i in range(half - 1)]
    far = [((i + 0.9) / half, half + i) for i in range(half)]
    return [0] + [k for _, k in sorted(near + far)]


def mate(me, k, count):
    found, bit = me, 1
    while bit < count:
        if k & bit:
            found = found + bit * (1 - 2 * lax.rem(lax.div(me, bit), 2))
        bit *= 2
    return found


def greet(me, tp, ep_count, tp_count):
    pairs = tp_count // 2
    pair, side = tp // 2, tp % 2
    barrier = pltpu.get_barrier_semaphore()
    for k in range(1, ep_count):
        pl.semaphore_signal(
            barrier,
            inc=1,
            device_id={"ep": lax.rem(me + k, ep_count), "tp": tp},
            device_id_type=MESH,
        )
    for j in range(1, pairs):
        pl.semaphore_signal(
            barrier,
            inc=1,
            device_id={"ep": me, "tp": lax.rem(pair + j, pairs) * 2 + side},
            device_id_type=MESH,
        )
    pl.semaphore_signal(
        barrier, inc=1, device_id={"ep": me, "tp": pair * 2 + 1 - side}, device_id_type=MESH
    )


def product(left, right, left_axis, right_axis):
    return lax.dot_general(
        left,
        right,
        (((left_axis,), (right_axis,)), ((), ())),
        preferred_element_type=wide,
    )


def iota(shape, axis):
    return lax.broadcasted_iota(jnp.int32, shape, axis)


def thirds(array):
    high = array.astype(kind)
    rest = array - high.astype(wide)
    middle = rest.astype(kind)
    return [high, middle, (rest - middle.astype(wide)).astype(kind)]


def kernel(
    ep_count,
    tp_count,
    query_ref,
    forget_ref,
    value_ref,
    opening_ref,
    margin_ref,
    surge_ref,
    head_gain_ref,
    tokens_ref,
    gain_ref,
    routes_ref,
    logits_ref,
    gate_hbm,
    up_hbm,
    down_hbm,
    matrix_hbm,
    mixed_ref,
    moe_ref,
    slots,
    piece,
    both,
    down,
    matrix,
    weights,
    lifted_ref,
    local_ref,
    window,
    window_total,
    before,
    before_total,
    outgoing,
    incoming,
    parts,
    mix,
    cbuf,
    cmix,
    ysend,
    ysmix,
    ybuf,
    ymix,
    abuf,
    returned,
    load,
    sa,
    ra,
    sy,
    ry,
    sc,
    rc,
    ss,
    rs,
    sb,
    rb,
    sz,
    rz,
    sh,
    rh,
):
    me, tp = lax.axis_index("ep"), lax.axis_index("tp")
    pairs = tp_count // 2
    pair, side = tp // 2, tp % 2
    other = pair * 2 + 1 - side
    order = visiting_order(ep_count)
    heads, seq_len = surge_ref.shape
    key_width = query_ref.shape[1] // heads
    value_width = value_ref.shape[1] // heads
    tok_rows, width = tokens_ref.shape
    capacity = slots.shape[1]
    units = gate_hbm.shape[0]
    offset = both.shape[0] // 2
    mix_rows = mix.shape[1]
    steps = outgoing.shape[0]
    half = ep_count * 5 // 8
    first, second = list(range(half)), list(range(half, ep_count))
    extra = ep_count
    whole_tiles = capacity % 16 == 0
    stride = min(width, 1024) if whole_tiles else width

    greet(me, tp, ep_count, tp_count)
    fetch = [
        pltpu.make_async_copy(gate_hbm, both.at[pl.ds(0, units)], load.at[0]),
        pltpu.make_async_copy(up_hbm, both.at[pl.ds(offset, units)], load.at[1]),
        pltpu.make_async_copy(down_hbm, down, load.at[2]),
        pltpu.make_async_copy(matrix_hbm, matrix, load.at[3]),
    ]
    for copy in fetch:
        copy.start()

    def remote(src, dst, send, recv, ep, to):
        return pltpu.make_async_remote_copy(
            src_ref=src,
            dst_ref=dst,
            send_sem=send,
            recv_sem=recv,
            device_id={"ep": ep, "tp": to},
            device_id_type=MESH,
        )

    def toward(j):
        return lax.rem(pair + j, pairs)

    def exchange(i):
        to = mate(me, order[i], ep_count)
        return remote(slots.at[i], piece.at[i, tp], sa.at[i], ra.at[i], to, tp)

    def across(i, j):
        to = toward(j) * 2 + side
        return remote(piece.at[i, tp], piece.at[i, tp], sy.at[j, i], ry.at[j, i], me, to)

    def beside(i, j):
        block = lax.rem(pair + pairs - j, pairs) * 2 + side
        return remote(
            piece.at[i, block], piece.at[i, block], sc.at[j, i], rc.at[j, i], me, other
        )

    def back_beside(i, j):
        block = toward(j) * 2 + 1 - side
        if i == extra:
            return remote(mix.at[block], cmix.at[j], sb.at[j, i], rb.at[j, i], me, other)
        return remote(parts.at[i, block], cbuf.at[j, i], sb.at[j, i], rb.at[j, i], me, other)

    def back_across(i, j):
        to = toward(j) * 2 + side
        if i == extra:
            return remote(ysmix.at[j], ymix.at[j], sz.at[j, i], rz.at[j, i], me, to)
        return remote(ysend.at[j, i], ybuf.at[j, i], sz.at[j, i], rz.at[j, i], me, to)

    def home(i):
        to = mate(me, order[i], ep_count)
        return remote(abuf.at[i], returned.at[i], sh.at[i], rh.at[i], to, tp)

    def pass_on(i):
        for j in range(1, pairs):
            across(i, j).start()
        beside(i, 0).start()

    def forward(i):
        exchange(i).wait_recv()
        pass_on(i)

    def relay(i):
        for j in range(1, pairs):
            across(i, j).wait_recv()
            beside(i, j).start()

    rows = tokens_ref[...].astype(wide)
    normed = (
        rows * lax.rsqrt(jnp.mean(rows * rows, axis=-1, keepdims=True) + epsilon) * gain_ref[...]
    ).astype(kind)
    listed = routes_ref[...]
    routes = listed[:, :tok_rows]
    for t in range(1, tp_count):
        routes = jnp.where(tp == t, listed[:, t * tok_rows : (t + 1) * tok_rows], routes)
    named = [routes[i : i + 1, :] for i in range(TOP)]
    experts = iota((ep_count, tok_rows), 0)
    tables = [(row == experts).astype(wide) for row in named]
    strict = (iota((tok_rows, tok_rows), 0) < iota((tok_rows, tok_rows), 1)).astype(kind)
    earlier = product(sum(tables).astype(kind), strict, 1, 0)
    places = [jnp.sum(earlier * table, axis=0, keepdims=True) for table in tables]
    spots = [row * capacity + place.astype(jnp.int32) for row, place in zip(named, places)]
    logits = logits_ref[...]
    raised = jnp.exp(logits - jnp.max(logits, axis=0, keepdims=True))
    share = raised / jnp.sum(raised, axis=0, keepdims=True)
    places_of = [
        iota((capacity, tok_rows), 0) + mate(me, k, ep_count) * capacity for k in order
    ]
    if whole_tiles:
        wanted = jnp.concatenate(places_of, axis=0)
        chooser = sum((spot == wanted).astype(wide) for spot in spots).astype(kind)
        for c in range(0, width, stride):
            cut = slice(c, c + stride)
            chosen = product(chooser, normed[:, cut], 1, 0).astype(kind)
            piece[0, tp, :, cut] = chosen[:capacity]
            for i in range(1, ep_count):
                slots[i, :, cut] = chosen[i * capacity : (i + 1) * capacity]
    else:
        for i, wanted in enumerate(places_of):
            chooser = sum((spot == wanted).astype(wide) for spot in spots).astype(kind)
            chosen = product(chooser, normed, 1, 0).astype(kind)
            if i:
                slots[i] = chosen
            else:
                piece[0, tp] = chosen
    pl.semaphore_wait(pltpu.get_barrier_semaphore(), ep_count + pairs - 1)
    pass_on(0)
    for i in range(1, ep_count):
        exchange(i).start()

    for i, wanted in enumerate(places_of):
        weight = sum(
            jnp.where(spot == wanted, share[r : r + 1, :], 0.0) for r, spot in enumerate(spots)
        )
        high = weight.astype(kind)
        low = (weight - high.astype(wide)).astype(kind)
        weights[0, i * capacity : (i + 1) * capacity, :] = high
        weights[1, i * capacity : (i + 1) * capacity, :] = low
    if units < offset:
        both[units:offset, :] = jnp.zeros((offset - units, width), kind)
        both[offset + units :, :] = jnp.zeros((offset - units, width), kind)

    at, since = iota((seq_len, seq_len), 0), iota((seq_len, seq_len), 1)
    shut = jax.nn.sigmoid(-forget_ref[...].astype(wide)) * margin_ref[...]
    within = ((at >= since) & (at // SPAN == since // SPAN)).astype(wide)
    running_all = sum(
        product(within.astype(kind), part, 1, 0) for part in thirds(jnp.log1p(-shut))
    )
    triangle = iota((SPAN, SPAN), 0) >= iota((SPAN, SPAN), 1)

    def recur(head):
        keys = slice(head * key_width, (head + 1) * key_width)
        values = slice(head * value_width, (head + 1) * value_width)
        surges = jnp.sum(within * surge_ref[head : head + 1, :], axis=1, keepdims=True)
        running_head = running_all[:, keys] + surges
        state = jnp.zeros((value_width, key_width), wide)
        total = jnp.zeros((1, key_width), wide)
        for span in range(seq_len // SPAN):
            part = slice(span * SPAN, (span + 1) * SPAN)
            running = running_head[part]
            closing = running[SPAN - 1 : SPAN]
            inflow = shut[part, keys]
            value = value_ref[part, values]
            query = query_ref[part, keys].astype(wide)
            lifted = (query * jnp.exp(running)).astype(kind)
            lowered = (inflow * jnp.exp(-running)).astype(kind)
            scores = jnp.where(triangle, product(lifted, lowered, 1, 1), 0.0)
            local = product(scores.astype(kind), value, 1, 0)
            if span:
                local = local + product(lifted, state.astype(kind), 1, 1)
            local_ref[part, values] = local
            lifted_ref[part, keys] = (query * jnp.exp(running + total)).astype(kind)
            fresh = product(value, (inflow * jnp.exp(closing - running)).astype(kind), 0, 0)
            state = jnp.exp(closing) * state + fresh
            total = total + closing
        window[head] = state
        window_total[head] = total

    def state_copy(step):
        to = lax.rem(me + 2**step, ep_count)
        return remote(outgoing.at[step], incoming.at[step], ss.at[step], rs.at[step], to, tp)

    def send_window(step):
        for head in range(heads):
            outgoing[step, head, :value_width] = window[head].astype(kind)
            total = window_total[head]
            coarse = total.astype(kind).astype(wide)
            line = iota((16, key_width), 0)
            tail = jnp.where(line == 0, coarse, jnp.where(line == 1, total - coarse, 0.0))
            outgoing[step, head, value_width:] = tail.astype(kind)

        @pl.when(me + 2**step < ep_count)
        def _():
            state_copy(step).start()

    def take_window(step):
        @pl.when(me >= 2**step)
        def _():
            state_copy(step).wait_recv()
            for head in range(heads):
                state = incoming[step, head, :value_width].astype(wide)
                total = jnp.sum(
                    incoming[step, head, value_width:].astype(wide), axis=0, keepdims=True
                )
                before[head] = jnp.exp(before_total[head]) * state + before[head]
                before_total[head] = before_total[head] + total
                window[head] = jnp.exp(window_total[head]) * state + window[head]
                window_total[head] = window_total[head] + total

    scanned = []

    def scan():
        if len(scanned) < steps:
            take_window(len(scanned))
            scanned.append(0)
            if len(scanned) < steps:
                send_window(len(scanned))

    def gathered(ref, group, sources=None):
        start, stop = group[0], group[-1] + 1
        if whole_tiles:
            return ref[start:stop].reshape(-1, width)
        if len(ref.shape) == 3:
            return jnp.concatenate([ref[i] for i in group], axis=0)
        return jnp.concatenate([ref[i, t] for i in group for t in range(tp_count)], axis=0)

    def arrive(group):
        for i in group:
            for j in range(pairs):
                beside(i, j).wait_recv()

    def raise_hidden(group):
        result = product(gathered(piece, group), both[...], 1, 1)
        left, right = result[:, :units], result[:, offset : offset + units]
        return (left * jax.nn.sigmoid(left) * right).astype(kind)

    def lower_hidden(group, hidden):
        start, stop = group[0], group[-1] + 1
        for c in range(0, width, stride):
            cut = slice(c, c + stride)
            result = product(hidden, down[:, cut], 1, 0).astype(kind)
            if whole_tiles:
                parts[start:stop, :, :, cut] = result.reshape(
                    stop - start, tp_count, capacity, stride
                )
            else:
                for n in range((stop - start) * tp_count):
                    i, t = start + n // tp_count, n % tp_count
                    parts[i, t, :, cut] = result[n * capacity : (n + 1) * capacity]

    def leaving(group):
        return sorted(group, key=lambda i: -order[i])

    def hand_over(group):
        for i in group:
            for j in list(range(1, pairs)) + [0]:
                back_beside(i, j).start()

    def fold(i):
        for j in range(1, pairs):
            back_beside(i, j).wait_recv()
            block = toward(j) * 2 + side
            if i == extra:
                ysmix[j] = (mix[block].astype(wide) + cmix[j].astype(wide)).astype(kind)
            else:
                ysend[j, i] = (parts[i, block].astype(wide) + cbuf[j, i].astype(wide)).astype(
                    kind
                )
            back_across(i, j).start()

    def settle(i):
        back_beside(i, 0).wait_recv()
        if i == extra:
            total = mix[tp].astype(wide) + cmix[0].astype(wide)
        else:
            total = parts[i, tp].astype(wide) + cbuf[0, i].astype(wide)
        for j in range(1, pairs):
            back_across(i, j).wait_recv()
            total = total + (ymix[j] if i == extra else ybuf[j, i]).astype(wide)
        total = total.astype(kind)
        if i == extra:
            mixed_ref[...] = total
        elif i == 0:
            returned[0] = total
        else:
            abuf[i] = total
            home(i).start()

    def combine(group):
        start, stop = group[0] * capacity, (group[-1] + 1) * capacity
        taken = gathered(returned, group)
        return product(weights[0, start:stop], taken, 0, 0) + product(
            weights[1, start:stop], taken, 0, 0
        )

    spare = len(second)
    quarter = max(1, spare // 4)
    chunks = [second[n : n + quarter] for n in range(0, spare, quarter)]

    def advance(group):
        for i in group:
            forward(i)
            relay(i - 1)

    recur(0)
    advance(first[1:2])
    for head in range(1, heads):
        recur(head)
    before[...] = jnp.zeros_like(before)
    before_total[...] = jnp.zeros_like(before_total)
    send_window(0)
    advance(first[2:])
    advance(chunks[0])
    arrive(first)
    for copy in fetch[:3]:
        copy.wait()
    hidden = raise_hidden(first)
    for chunk in chunks[1:2]:
        advance(chunk)
    scan()
    lower_hidden(first, hidden)
    hand_over(leaving(first))
    for chunk in chunks[2:]:
        advance(chunk)
    for i in leaving(first):
        fold(i)
    relay(ep_count - 1)
    scan()
    arrive(second)
    hidden = raise_hidden(second)
    lower_hidden(second, hidden)
    hand_over(leaving(second))
    for i in leaving(first)[:2]:
        settle(i)
    for i in leaving(second):
        fold(i)
    for _ in range(steps):
        scan()
    for head in range(heads):
        keys = slice(head * key_width, (head + 1) * key_width)
        values = slice(head * value_width, (head + 1) * value_width)
        out = local_ref[:, values] + product(
            lifted_ref[:, keys], before[head].astype(kind), 1, 1
        )
        out = out * lax.rsqrt(jnp.mean(out * out, axis=-1, keepdims=True) + epsilon)
        opening = opening_ref[:, values].astype(wide)
        lifted_ref[:, values] = (
            out * head_gain_ref[:, values] * (opening * jax.nn.sigmoid(opening))
        ).astype(kind)
    fetch[3].wait()
    for c in range(0, width, stride):
        cut = slice(c, c + stride)
        result = product(lifted_ref[...], matrix[:, cut], 1, 0).astype(kind)
        mix[:, :, cut] = result.reshape(tp_count, mix_rows, stride)
    hand_over([extra])
    for i in leaving(first)[2:]:
        settle(i)
    fold(extra)
    for i in leaving(second):
        settle(i)
    for i in first[1:]:
        home(i).wait_recv()
    total = combine(first)
    for i in second:
        home(i).wait_recv()
    moe_ref[...] = (total + combine(second)).astype(kind)
    settle(extra)

    for i in range(ep_count):
        if i:
            exchange(i).wait_send()
            home(i).wait_send()
    for i in range(ep_count + 1):
        for j in range(pairs):
            back_beside(i, j).wait_send()
            if j:
                back_across(i, j).wait_send()
            if i < ep_count:
                beside(i, j).wait_send()
                if j:
                    across(i, j).wait_send()
    for step in range(steps):

        @pl.when(me + 2**step < ep_count)
        def _(step=step):
            state_copy(step).wait_send()


def run(small, large, heads, capacity, ep_count, tp_count):
    pairs = tp_count // 2
    dma = pltpu.SemaphoreType.DMA
    vmem = pl.BlockSpec(memory_space=pltpu.VMEM)
    hbm = pl.BlockSpec(memory_space=pl.ANY)
    query, value, tokens = small[0], small[2], small[7]
    gate, _, down, matrix = large
    seq_len, keys = query.shape
    values = value.shape[1]
    tok_rows, width = tokens.shape
    units = gate.shape[0]
    padded = -(-units // 128) * 128
    key_width, value_width = keys // heads, values // heads
    steps = (ep_count - 1).bit_length()
    mix_rows = seq_len // tp_count
    chunks = (ep_count, capacity, width)
    many = (pairs, ep_count + 1)
    state = (steps, heads, value_width + 16, key_width)
    return pl.pallas_call(
        functools.partial(kernel, ep_count, tp_count),
        out_shape=(
            jax.ShapeDtypeStruct((mix_rows, width), kind),
            jax.ShapeDtypeStruct((tok_rows, width), kind),
        ),
        in_specs=[vmem] * len(small) + [hbm] * len(large),
        out_specs=(vmem, vmem),
        scratch_shapes=[
            pltpu.VMEM(chunks, kind),
            pltpu.VMEM((ep_count, tp_count, capacity, width), kind),
            pltpu.VMEM((2 * padded, width), kind),
            pltpu.VMEM(down.shape, kind),
            pltpu.VMEM(matrix.shape, kind),
            pltpu.VMEM((2, ep_count * capacity, tok_rows), kind),
            pltpu.VMEM((seq_len, keys), kind),
            pltpu.VMEM((seq_len, values), wide),
            pltpu.VMEM((heads, value_width, key_width), wide),
            pltpu.VMEM((heads, 1, key_width), wide),
            pltpu.VMEM((heads, value_width, key_width), wide),
            pltpu.VMEM((heads, 1, key_width), wide),
            pltpu.VMEM(state, kind),
            pltpu.VMEM(state, kind),
            pltpu.VMEM((ep_count, tp_count, capacity, width), kind),
            pltpu.VMEM((tp_count, mix_rows, width), kind),
            pltpu.VMEM((pairs,) + chunks, kind),
            pltpu.VMEM((pairs, mix_rows, width), kind),
            pltpu.VMEM((pairs,) + chunks, kind),
            pltpu.VMEM((pairs, mix_rows, width), kind),
            pltpu.VMEM((pairs,) + chunks, kind),
            pltpu.VMEM((pairs, mix_rows, width), kind),
            pltpu.VMEM(chunks, kind),
            pltpu.VMEM(chunks, kind),
            dma((4,)),
            dma((ep_count,)),
            dma((ep_count,)),
            dma(many),
            dma(many),
            dma(many),
            dma(many),
            dma((steps,)),
            dma((steps,)),
            dma(many),
            dma(many),
            dma(many),
            dma(many),
            dma((ep_count,)),
            dma((ep_count,)),
        ],
        compiler_params=pltpu.CompilerParams(
            collective_id=0, has_side_effects=True, vmem_limit_bytes=60 << 20
        ),
    )(*small, *large)


def per_device(
    recurrence_query,
    forget_preactivation,
    recurrence_value,
    output_gate_preactivation,
    forget_margin,
    surge_log_decay,
    head_norm_gain,
    recurrence_output_matrix,
    second_micro_input,
    expert_norm_gain,
    routes,
    router_chosen_logits,
    expert_gate_matrix,
    expert_up_matrix,
    expert_down_matrix,
):
    tp_count = lax.axis_size("tp")
    expert_count = lax.axis_size("ep")
    tok_rows = second_micro_input.shape[0]
    capacity = 2 * tok_rows * TOP // expert_count
    small = (
        recurrence_query,
        forget_preactivation,
        recurrence_value,
        output_gate_preactivation,
        forget_margin[None, :],
        surge_log_decay,
        head_norm_gain[None, :],
        second_micro_input,
        expert_norm_gain[None, :],
        routes.T,
        router_chosen_logits.T,
    )
    large = (
        expert_gate_matrix[0].T,
        expert_up_matrix[0].T,
        expert_down_matrix[0],
        recurrence_output_matrix,
    )
    return run(small, large, surge_log_decay.shape[0], capacity, expert_count, tp_count)


def solution(mesh):
    return jax.shard_map(
        per_device,
        mesh=mesh,
        in_specs=(
            P("ep", "tp"),
            P("ep", "tp"),
            P("ep", "tp"),
            P("ep", "tp"),
            P("tp"),
            P("tp", "ep"),
            P("tp"),
            P("tp", None),
            P(("ep", "tp"), None),
            P(),
            P("ep", None),
            P(("ep", "tp"), None),
            P("ep", None, "tp"),
            P("ep", None, "tp"),
            P("ep", "tp", None),
        ),
        out_specs=(P(("ep", "tp"), None), P(("ep", "tp"), None)),
        check_vma=False,
    )
```

```python
import functools

import jax
import jax.numpy as jnp
from jax import lax
from jax.experimental import pallas as pl
from jax.experimental.pallas import tpu as pltpu
from jax.sharding import PartitionSpec as P

TOP = 2
SPAN = 64
MESH = pl.DeviceIdType.MESH


epsilon = 1e-06
wide = jnp.float32
kind = jnp.bfloat16


def visiting_order(count):
    half = count // 2
    near = [(i / max(1, half - 1), i + 1) for i in range(half - 1)]
    far = [((i + 0.9) / half, half + i) for i in range(half)]
    return [0] + [k for _, k in sorted(near + far)]


def mate(me, k, count):
    found, bit = me, 1
    while bit < count:
        if k & bit:
            found = found + bit * (1 - 2 * lax.rem(lax.div(me, bit), 2))
        bit *= 2
    return found


def greet(me, tp, ep_count, tp_count):
    pairs = tp_count // 2
    pair, side = tp // 2, tp % 2
    barrier = pltpu.get_barrier_semaphore()
    for k in range(1, ep_count):
        pl.semaphore_signal(
            barrier,
            inc=1,
            device_id={"ep": lax.rem(me + k, ep_count), "tp": tp},
            device_id_type=MESH,
        )
    for j in range(1, pairs):
        pl.semaphore_signal(
            barrier,
            inc=1,
            device_id={"ep": me, "tp": lax.rem(pair + j, pairs) * 2 + side},
            device_id_type=MESH,
        )
    pl.semaphore_signal(
        barrier, inc=1, device_id={"ep": me, "tp": pair * 2 + 1 - side}, device_id_type=MESH
    )


def product(left, right, left_axis, right_axis):
    return lax.dot_general(
        left,
        right,
        (((left_axis,), (right_axis,)), ((), ())),
        preferred_element_type=wide,
    )


def iota(shape, axis):
    return lax.broadcasted_iota(jnp.int32, shape, axis)


def thirds(array):
    high = array.astype(kind)
    rest = array - high.astype(wide)
    middle = rest.astype(kind)
    return [high, middle, (rest - middle.astype(wide)).astype(kind)]


def kernel(
    ep_count,
    tp_count,
    query_ref,
    forget_ref,
    value_ref,
    opening_ref,
    margin_ref,
    surge_ref,
    head_gain_ref,
    tokens_ref,
    gain_ref,
    routes_ref,
    logits_ref,
    gate_hbm,
    up_hbm,
    down_hbm,
    matrix_hbm,
    mixed_ref,
    moe_ref,
    slots,
    piece,
    both,
    turned,
    down,
    matrix,
    weights,
    note,
    notes,
    guest_weights,
    lifted_ref,
    local_ref,
    window,
    window_total,
    before,
    before_total,
    outgoing,
    incoming,
    parts,
    mix,
    cbuf,
    cmix,
    ysend,
    ysmix,
    ybuf,
    ymix,
    abuf,
    returned,
    guest_abuf,
    guest_returned,
    crossing,
    crossed,
    load,
    sa,
    ra,
    sy,
    ry,
    sc,
    rc,
    ss,
    rs,
    sb,
    rb,
    sz,
    rz,
    sh,
    rh,
    sg,
    rg,
    sn,
    rn,
    su,
    ru,
):
    me, tp = lax.axis_index("ep"), lax.axis_index("tp")
    pairs = tp_count // 2
    pair, side = tp // 2, tp % 2
    other = pair * 2 + 1 - side
    order = visiting_order(ep_count)
    heads, seq_len = surge_ref.shape
    key_width = query_ref.shape[1] // heads
    value_width = value_ref.shape[1] // heads
    tok_rows, width = tokens_ref.shape
    capacity = slots.shape[1]
    units = gate_hbm.shape[0]
    offset = both.shape[0] // 2
    mix_rows = mix.shape[1]
    steps = outgoing.shape[0]
    cuts = (0, ep_count // 2, ep_count * 7 // 8, ep_count)
    first, second, third = [list(range(*cuts[n : n + 2])) for n in range(3)]
    extra = ep_count
    near = [i for i in range(ep_count) if 2 * order[i] < ep_count]
    distant = [i for i in range(ep_count) if i not in near]
    whole_tiles = capacity % 16 == 0
    stride = min(width, 1024) if whole_tiles else width

    greet(me, tp, ep_count, tp_count)
    fetch = [
        pltpu.make_async_copy(gate_hbm, both.at[pl.ds(0, units)], load.at[0]),
        pltpu.make_async_copy(up_hbm, both.at[pl.ds(offset, units)], load.at[1]),
        pltpu.make_async_copy(down_hbm, down, load.at[2]),
        pltpu.make_async_copy(matrix_hbm, matrix, load.at[3]),
    ]
    for copy in fetch:
        copy.start()

    def remote(src, dst, send, recv, ep, to):
        return pltpu.make_async_remote_copy(
            src_ref=src,
            dst_ref=dst,
            send_sem=send,
            recv_sem=recv,
            device_id={"ep": ep, "tp": to},
            device_id_type=MESH,
        )

    def toward(j):
        return lax.rem(pair + j, pairs)

    def exchange(i):
        to = mate(me, order[i], ep_count)
        return remote(slots.at[i], piece.at[i, tp], sa.at[i], ra.at[i], to, tp)

    def across(i, j):
        to = toward(j) * 2 + side
        return remote(piece.at[i, tp], piece.at[i, tp], sy.at[j, i], ry.at[j, i], me, to)

    def beside(i, j):
        block = lax.rem(pair + pairs - j, pairs) * 2 + side
        return remote(
            piece.at[i, block], piece.at[i, block], sc.at[j, i], rc.at[j, i], me, other
        )

    def back_beside(i, j):
        block = toward(j) * 2 + 1 - side
        if i == extra:
            return remote(mix.at[block], cmix.at[j], sb.at[j, i], rb.at[j, i], me, other)
        return remote(parts.at[i, block], cbuf.at[j, i], sb.at[j, i], rb.at[j, i], me, other)

    def back_across(i, j):
        to = toward(j) * 2 + side
        if i == extra:
            return remote(ysmix.at[j], ymix.at[j], sz.at[j, i], rz.at[j, i], me, to)
        return remote(ysend.at[j, i], ybuf.at[j, i], sz.at[j, i], rz.at[j, i], me, to)

    def home(i):
        to = mate(me, order[i], ep_count)
        return remote(abuf.at[i], returned.at[i], sh.at[i], rh.at[i], to, tp)

    def tell(j):
        return remote(note, notes.at[j], sn.at[j], rn.at[j], me, toward(j) * 2 + side)

    def home_guest(i, j):
        to = mate(me, order[i], ep_count)
        at = near.index(i)
        return remote(
            guest_abuf.at[j, at], guest_returned.at[j, at], sg.at[j, i], rg.at[j, i], to, tp
        )

    def cross(j):
        to = toward(j) * 2 + side
        return remote(crossing.at[j], crossed.at[j], su.at[j], ru.at[j], me, to)

    def back_beside(i, j):
        block = toward(j) * 2 + 1 - side
        if i == extra:
            return remote(mix.at[block], cmix.at[j], sb.at[j, i], rb.at[j, i], me, other)
        return remote(parts.at[i, block], cbuf.at[j, i], sb.at[j, i], rb.at[j, i], me, other)

    def back_across(i, j):
        to = toward(j) * 2 + side
        if i == extra:
            return remote(ysmix.at[j], ymix.at[j], sz.at[j, i], rz.at[j, i], me, to)
        return remote(ysend.at[j, i], ybuf.at[j, i], sz.at[j, i], rz.at[j, i], me, to)

    def home(i):
        to = mate(me, order[i], ep_count)
        return remote(abuf.at[i], returned.at[i], sh.at[i], rh.at[i], to, tp)

    def pass_on(i):
        for j in range(1, pairs):
            across(i, j).start()
        beside(i, 0).start()

    def forward(i):
        exchange(i).wait_recv()
        pass_on(i)

    def relay(i):
        for j in range(1, pairs):
            across(i, j).wait_recv()
            beside(i, j).start()

    rows = tokens_ref[...].astype(wide)
    normed = (
        rows * lax.rsqrt(jnp.mean(rows * rows, axis=-1, keepdims=True) + epsilon) * gain_ref[...]
    ).astype(kind)
    listed = routes_ref[...]
    experts = iota((ep_count, tok_rows), 0)
    strict = (iota((tok_rows, tok_rows), 0) < iota((tok_rows, tok_rows), 1)).astype(kind)

    def spots_of(index):
        routes = listed[:, :tok_rows]
        for t in range(1, tp_count):
            routes = jnp.where(index == t, listed[:, t * tok_rows : (t + 1) * tok_rows], routes)
        named = [routes[i : i + 1, :] for i in range(TOP)]
        tables = [(row == experts).astype(wide) for row in named]
        earlier = product(sum(tables).astype(kind), strict, 1, 0)
        places = [jnp.sum(earlier * table, axis=0, keepdims=True) for table in tables]
        return [row * capacity + place.astype(jnp.int32) for row, place in zip(named, places)]

    places_of = [
        iota((capacity, tok_rows), 0) + mate(me, k, ep_count) * capacity for k in order
    ]

    def choose(spots, tokens, members, store):
        if whole_tiles:
            wanted = jnp.concatenate([places_of[i] for i in members], axis=0)
            chooser = sum((spot == wanted).astype(wide) for spot in spots).astype(kind)
            for c in range(0, width, stride):
                cut = slice(c, c + stride)
                chosen = product(chooser, tokens[:, cut], 1, 0).astype(kind)
                for n, i in enumerate(members):
                    store(i, cut, chosen[n * capacity : (n + 1) * capacity])
        else:
            for i in members:
                chooser = sum((spot == places_of[i]).astype(wide) for spot in spots)
                store(i, slice(None), product(chooser.astype(kind), tokens, 1, 0).astype(kind))

    def keep(i, cut, rows):
        if i:
            slots[i, :, cut] = rows
        else:
            piece[i, tp, :, cut] = rows

    spots = spots_of(tp)
    choose(spots, normed, range(ep_count), keep)
    pl.semaphore_wait(pltpu.get_barrier_semaphore(), ep_count + pairs - 1)
    pass_on(0)
    for i in range(1, ep_count):
        exchange(i).start()

    def share_of(logits):
        raised = jnp.exp(logits - jnp.max(logits, axis=0, keepdims=True))
        return raised / jnp.sum(raised, axis=0, keepdims=True)

    def weigh(spots, share, members, store):
        for i in members:
            weight = sum(
                jnp.where(spot == places_of[i], share[r : r + 1, :], 0.0)
                for r, spot in enumerate(spots)
            )
            high = weight.astype(kind)
            store(i, high, (weight - high.astype(wide)).astype(kind))

    def keep_weight(i, high, low):
        weights[0, i * capacity : (i + 1) * capacity, :] = high
        weights[1, i * capacity : (i + 1) * capacity, :] = low

    note[...] = jnp.zeros_like(note)
    note[:TOP, :tok_rows] = logits_ref[...]
    for j in range(1, pairs):
        tell(j).start()
    weigh(spots, share_of(logits_ref[...]), range(ep_count), keep_weight)
    if units < offset:
        both[units:offset, :] = jnp.zeros((offset - units, width), kind)
        both[offset + units :, :] = jnp.zeros((offset - units, width), kind)

    at, since = iota((seq_len, seq_len), 0), iota((seq_len, seq_len), 1)
    shut = jax.nn.sigmoid(-forget_ref[...].astype(wide)) * margin_ref[...]
    within = ((at >= since) & (at // SPAN == since // SPAN)).astype(wide)
    running_all = sum(
        product(within.astype(kind), part, 1, 0) for part in thirds(jnp.log1p(-shut))
    )
    triangle = iota((SPAN, SPAN), 0) >= iota((SPAN, SPAN), 1)

    def recur(head):
        keys = slice(head * key_width, (head + 1) * key_width)
        values = slice(head * value_width, (head + 1) * value_width)
        surges = jnp.sum(within * surge_ref[head : head + 1, :], axis=1, keepdims=True)
        running_head = running_all[:, keys] + surges
        state = jnp.zeros((value_width, key_width), wide)
        total = jnp.zeros((1, key_width), wide)
        for span in range(seq_len // SPAN):
            part = slice(span * SPAN, (span + 1) * SPAN)
            running = running_head[part]
            closing = running[SPAN - 1 : SPAN]
            inflow = shut[part, keys]
            value = value_ref[part, values]
            query = query_ref[part, keys].astype(wide)
            lifted = (query * jnp.exp(running)).astype(kind)
            lowered = (inflow * jnp.exp(-running)).astype(kind)
            scores = jnp.where(triangle, product(lifted, lowered, 1, 1), 0.0)
            local = product(scores.astype(kind), value, 1, 0)
            if span:
                local = local + product(lifted, state.astype(kind), 1, 1)
            local_ref[part, values] = local
            lifted_ref[part, keys] = (query * jnp.exp(running + total)).astype(kind)
            fresh = product(value, (inflow * jnp.exp(closing - running)).astype(kind), 0, 0)
            state = jnp.exp(closing) * state + fresh
            total = total + closing
        window[head] = state
        window_total[head] = total

    def state_copy(step):
        to = lax.rem(me + 2**step, ep_count)
        return remote(outgoing.at[step], incoming.at[step], ss.at[step], rs.at[step], to, tp)

    def send_window(step):
        for head in range(heads):
            outgoing[step, head, :value_width] = window[head].astype(kind)
            total = window_total[head]
            coarse = total.astype(kind).astype(wide)
            line = iota((16, key_width), 0)
            tail = jnp.where(line == 0, coarse, jnp.where(line == 1, total - coarse, 0.0))
            outgoing[step, head, value_width:] = tail.astype(kind)

        @pl.when(me + 2**step < ep_count)
        def _():
            state_copy(step).start()

    def take_window(step):
        @pl.when(me >= 2**step)
        def _():
            state_copy(step).wait_recv()
            for head in range(heads):
                state = incoming[step, head, :value_width].astype(wide)
                total = jnp.sum(
                    incoming[step, head, value_width:].astype(wide), axis=0, keepdims=True
                )
                before[head] = jnp.exp(before_total[head]) * state + before[head]
                before_total[head] = before_total[head] + total
                window[head] = jnp.exp(window_total[head]) * state + window[head]
                window_total[head] = window_total[head] + total

    scanned = []

    def scan():
        if len(scanned) < steps:
            take_window(len(scanned))
            scanned.append(0)
            if len(scanned) < steps:
                send_window(len(scanned))

    def gathered(ref, group, sources=None):
        start, stop = group[0], group[-1] + 1
        if whole_tiles:
            return ref[start:stop].reshape(-1, width)
        if len(ref.shape) == 3:
            return jnp.concatenate([ref[i] for i in group], axis=0)
        return jnp.concatenate([ref[i, t] for i in group for t in range(tp_count)], axis=0)

    def arrive(group):
        for i in group:
            for j in range(pairs):
                beside(i, j).wait_recv()

    def raise_hidden(group):
        result = product(gathered(piece, group), turned[...], 1, 0)
        left, right = result[:, :units], result[:, offset : offset + units]
        return (left * jax.nn.sigmoid(left) * right).astype(kind)

    def lower_hidden(group, hidden):
        start, stop = group[0], group[-1] + 1
        for c in range(0, width, stride):
            cut = slice(c, c + stride)
            result = product(hidden, down[:, cut], 1, 0).astype(kind)
            if whole_tiles:
                parts[start:stop, :, :, cut] = result.reshape(
                    stop - start, tp_count, capacity, stride
                )
            else:
                for n in range((stop - start) * tp_count):
                    i, t = start + n // tp_count, n % tp_count
                    parts[i, t, :, cut] = result[n * capacity : (n + 1) * capacity]

    def leaving(group):
        return sorted(group, key=lambda i: -order[i])

    def hand_over(group):
        for i in group:
            for j in list(range(1, pairs)) + [0]:
                back_beside(i, j).start()

    def fold(i):
        for j in range(1, pairs):
            back_beside(i, j).wait_recv()
            block = toward(j) * 2 + side
            if i == extra:
                ysmix[j] = (mix[block].astype(wide) + cmix[j].astype(wide)).astype(kind)
            else:
                ysend[j, i] = (parts[i, block].astype(wide) + cbuf[j, i].astype(wide)).astype(
                    kind
                )
            back_across(i, j).start()

    def settle(i):
        back_beside(i, 0).wait_recv()
        if i == extra:
            total = mix[tp].astype(wide) + cmix[0].astype(wide)
        else:
            total = parts[i, tp].astype(wide) + cbuf[0, i].astype(wide)
        for j in range(1, pairs):
            back_across(i, j).wait_recv()
            total = total + (ymix[j] if i == extra else ybuf[j, i]).astype(wide)
        if i == extra:
            mixed_ref[...] = total.astype(kind)
        else:
            abuf[i] = total.astype(kind)
            home(i).start()

    def settle_near(i):
        for j in range(1, pairs):
            back_beside(i, j).wait_recv()
            block = toward(j) * 2 + side
            total = (parts[i, block].astype(wide) + cbuf[j, i].astype(wide)).astype(kind)
            if i == 0:
                guest_returned[j, near.index(0)] = total
            else:
                guest_abuf[j, near.index(i)] = total
                home_guest(i, j).start()
        back_beside(i, 0).wait_recv()
        total = (parts[i, tp].astype(wide) + cbuf[0, i].astype(wide)).astype(kind)
        if i == 0:
            returned[i] = total
        else:
            abuf[i] = total
            home(i).start()

    def combine(ref, group, scale):
        start, stop = group[0] * capacity, (group[-1] + 1) * capacity
        taken = gathered(ref, group)
        return product(scale[0, start:stop], taken, 0, 0) + product(
            scale[1, start:stop], taken, 0, 0
        )

    def expert(group):
        arrive(group)
        lower_hidden(group, raise_hidden(group))
        hand_over(group)

    def advance(group):
        for i in group:
            forward(i)
            relay(i - 1)

    def far(group):
        return [i for i in leaving(group) if i in distant]

    def close(group):
        return [i for i in leaving(group) if i in near]

    def fold_all(group):
        for i in group:
            fold(i)

    def settle_all(group):
        for i in group:
            settle(i)

    def settle_close(group):
        for i in close(group):
            settle_near(i)

    def keep_guest_weight(i, high, low):
        at = near.index(i) * capacity
        guest_weights[0, at : at + capacity, :] = high
        guest_weights[1, at : at + capacity, :] = low

    bands = [slice(n, n + 128) for n in range(0, 2 * offset, 128)]
    third_part = -(-len(bands) // 3)

    def turn(part):
        for band in bands[part * third_part : (part + 1) * third_part]:
            turned[:, band] = both[band, :].T

    recur(0)
    advance(first[1:2])
    for head in range(1, heads):
        recur(head)
    before[...] = jnp.zeros_like(before)
    before_total[...] = jnp.zeros_like(before_total)
    send_window(0)
    for copy in fetch[:2]:
        copy.wait()
    turn(0)
    advance(first[2:3])
    turn(1)
    advance(first[3:])
    turn(2)
    advance(second[:1])
    arrive(first)
    fetch[2].wait()
    hidden = raise_hidden(first)
    advance(second[1:2])
    lower_hidden(first, hidden)
    hand_over(far(first) + close(first))
    advance(second[2:])
    fold_all(far(first)[-1:])
    settle_close(first)
    scan()
    advance(third)
    fold_all(far(first)[:-1])
    arrive(second)
    hidden = raise_hidden(second)
    lower_hidden(second, hidden)
    hand_over(far(second) + close(second))
    settle_all(far(first)[-1:])
    fold_all(far(second))
    relay(ep_count - 1)
    scan()
    settle_all(far(first)[:-1])
    expert(third)
    settle_close(second)
    fold_all(far(third))
    settle_close(third)
    settle_all(far(second))
    for _ in range(steps):
        scan()
    for head in range(heads):
        keys = slice(head * key_width, (head + 1) * key_width)
        values = slice(head * value_width, (head + 1) * value_width)
        out = local_ref[:, values] + product(
            lifted_ref[:, keys], before[head].astype(kind), 1, 1
        )
        out = out * lax.rsqrt(jnp.mean(out * out, axis=-1, keepdims=True) + epsilon)
        opening = opening_ref[:, values].astype(wide)
        lifted_ref[:, values] = (
            out * head_gain_ref[:, values] * (opening * jax.nn.sigmoid(opening))
        ).astype(kind)
    fetch[3].wait()
    for c in range(0, width, stride):
        cut = slice(c, c + stride)
        result = product(lifted_ref[...], matrix[:, cut], 1, 0).astype(kind)
        mix[:, :, cut] = result.reshape(tp_count, mix_rows, stride)
    hand_over([extra])
    fold(extra)
    for j in range(1, pairs):
        tell(j).wait_recv()
        weigh(
            spots_of(toward(j) * 2 + side),
            share_of(notes[pairs - j][:TOP, :tok_rows]),
            near,
            keep_guest_weight,
        )
        for i in near:
            if i:
                home_guest(i, j).wait_recv()
        crossing[j] = combine(guest_returned.at[j], range(len(near)), guest_weights).astype(kind)
        cross(j).start()
    settle_all(far(third))
    for i in first[1:] + second:
        home(i).wait_recv()
    total = combine(returned, first + second, weights)
    settle(extra)
    for i in third:
        home(i).wait_recv()
    total = total + combine(returned, third, weights)
    for j in range(1, pairs):
        cross(j).wait_recv()
        total = total + crossed[j].astype(wide)
    moe_ref[...] = total.astype(kind)

    for i in range(ep_count):
        if i:
            exchange(i).wait_send()
            home(i).wait_send()
    for j in range(1, pairs):
        tell(j).wait_send()
        cross(j).wait_send()
        for i in near:
            if i:
                home_guest(i, j).wait_send()
        for i in distant + [extra]:
            back_across(i, j).wait_send()
        for i in range(ep_count):
            across(i, j).wait_send()
    for i in range(ep_count + 1):
        for j in range(pairs):
            back_beside(i, j).wait_send()
            if i < ep_count:
                beside(i, j).wait_send()
    for step in range(steps):

        @pl.when(me + 2**step < ep_count)
        def _(step=step):
            state_copy(step).wait_send()


def run(small, large, heads, capacity, ep_count, tp_count):
    pairs = tp_count // 2
    dma = pltpu.SemaphoreType.DMA
    vmem = pl.BlockSpec(memory_space=pltpu.VMEM)
    hbm = pl.BlockSpec(memory_space=pl.ANY)
    query, value, tokens = small[0], small[2], small[7]
    gate, _, down, matrix = large
    seq_len, keys = query.shape
    values = value.shape[1]
    tok_rows, width = tokens.shape
    units = gate.shape[0]
    padded = -(-units // 128) * 128
    key_width, value_width = keys // heads, values // heads
    steps = (ep_count - 1).bit_length()
    mix_rows = seq_len // tp_count
    chunks = (ep_count, capacity, width)
    many = (pairs, ep_count + 1)
    nearby = (ep_count // 2, capacity, width)
    state = (steps, heads, value_width + 16, key_width)
    return pl.pallas_call(
        functools.partial(kernel, ep_count, tp_count),
        out_shape=(
            jax.ShapeDtypeStruct((mix_rows, width), kind),
            jax.ShapeDtypeStruct((tok_rows, width), kind),
        ),
        in_specs=[vmem] * len(small) + [hbm] * len(large),
        out_specs=(vmem, vmem),
        scratch_shapes=[
            pltpu.VMEM(chunks, kind),
            pltpu.VMEM((ep_count, tp_count, capacity, width), kind),
            pltpu.VMEM((2 * padded, width), kind),
            pltpu.VMEM((width, 2 * padded), kind),
            pltpu.VMEM(down.shape, kind),
            pltpu.VMEM(matrix.shape, kind),
            pltpu.VMEM((2, ep_count * capacity, tok_rows), kind),
            pltpu.VMEM((8, 128), wide),
            pltpu.VMEM((pairs, 8, 128), wide),
            pltpu.VMEM((2, nearby[0] * capacity, tok_rows), kind),
            pltpu.VMEM((seq_len, keys), kind),
            pltpu.VMEM((seq_len, values), wide),
            pltpu.VMEM((heads, value_width, key_width), wide),
            pltpu.VMEM((heads, 1, key_width), wide),
            pltpu.VMEM((heads, value_width, key_width), wide),
            pltpu.VMEM((heads, 1, key_width), wide),
            pltpu.VMEM(state, kind),
            pltpu.VMEM(state, kind),
            pltpu.VMEM((ep_count, tp_count, capacity, width), kind),
            pltpu.VMEM((tp_count, mix_rows, width), kind),
            pltpu.VMEM((pairs,) + chunks, kind),
            pltpu.VMEM((pairs, mix_rows, width), kind),
            pltpu.VMEM((pairs,) + chunks, kind),
            pltpu.VMEM((pairs, mix_rows, width), kind),
            pltpu.VMEM((pairs,) + chunks, kind),
            pltpu.VMEM((pairs, mix_rows, width), kind),
            pltpu.VMEM(chunks, kind),
            pltpu.VMEM(chunks, kind),
            pltpu.VMEM((pairs,) + nearby, kind),
            pltpu.VMEM((pairs,) + nearby, kind),
            pltpu.VMEM((pairs, tok_rows, width), kind),
            pltpu.VMEM((pairs, tok_rows, width), kind),
            dma((4,)),
            dma((ep_count,)),
            dma((ep_count,)),
            dma(many),
            dma(many),
            dma(many),
            dma(many),
            dma((steps,)),
            dma((steps,)),
            dma(many),
            dma(many),
            dma(many),
            dma(many),
            dma((ep_count,)),
            dma((ep_count,)),
            dma(many),
            dma(many),
            dma((pairs,)),
            dma((pairs,)),
            dma((pairs,)),
            dma((pairs,)),
        ],
        compiler_params=pltpu.CompilerParams(
            collective_id=0, has_side_effects=True, vmem_limit_bytes=60 << 20
        ),
    )(*small, *large)


def hand_out_kernel(mixed_in, moe_in, mixed_out, moe_out):
    mixed_out[...] = mixed_in[...]
    moe_out[...] = moe_in[...]


def hand_out(mixed, moe):
    vmem = pl.BlockSpec(memory_space=pltpu.VMEM)
    return pl.pallas_call(
        hand_out_kernel,
        out_shape=tuple(jax.ShapeDtypeStruct(part.shape, part.dtype) for part in (mixed, moe)),
        in_specs=[vmem] * 2,
        out_specs=(vmem, vmem),
    )(mixed, moe)


def per_device(
    recurrence_query,
    forget_preactivation,
    recurrence_value,
    output_gate_preactivation,
    forget_margin,
    surge_log_decay,
    head_norm_gain,
    recurrence_output_matrix,
    second_micro_input,
    expert_norm_gain,
    routes,
    router_chosen_logits,
    expert_gate_matrix,
    expert_up_matrix,
    expert_down_matrix,
):
    tp_count = lax.axis_size("tp")
    expert_count = lax.axis_size("ep")
    tok_rows = second_micro_input.shape[0]
    capacity = 2 * tok_rows * TOP // expert_count
    small = (
        recurrence_query,
        forget_preactivation,
        recurrence_value,
        output_gate_preactivation,
        forget_margin[None, :],
        surge_log_decay,
        head_norm_gain[None, :],
        second_micro_input,
        expert_norm_gain[None, :],
        routes.T,
        router_chosen_logits.T,
    )
    large = (
        expert_gate_matrix[0].T,
        expert_up_matrix[0].T,
        expert_down_matrix[0],
        recurrence_output_matrix,
    )
    heads = surge_log_decay.shape[0]
    return hand_out(*run(small, large, heads, capacity, expert_count, tp_count))


def solution(mesh):
    return jax.shard_map(
        per_device,
        mesh=mesh,
        in_specs=(
            P("ep", "tp"),
            P("ep", "tp"),
            P("ep", "tp"),
            P("ep", "tp"),
            P("tp"),
            P("tp", "ep"),
            P("tp"),
            P("tp", None),
            P(("ep", "tp"), None),
            P(),
            P("ep", None),
            P(("ep", "tp"), None),
            P("ep", None, "tp"),
            P("ep", None, "tp"),
            P("ep", "tp", None),
        ),
        out_specs=(P(("ep", "tp"), None), P(("ep", "tp"), None)),
        check_vma=False,
    )
```

```python
import functools

import jax
import jax.numpy as jnp
from jax import lax
from jax.experimental import pallas as pl
from jax.experimental.pallas import tpu as pltpu
from jax.sharding import PartitionSpec as P

TOP = 2
SPAN = 64
MESH = pl.DeviceIdType.MESH


epsilon = 1e-06
wide = jnp.float32
kind = jnp.bfloat16


def visiting_order(count):
    half = count // 2
    near = [(i / max(1, half - 1), i + 1) for i in range(half - 1)]
    far = [((i + 0.9) / half, half + i) for i in range(half)]
    return [0] + [k for _, k in sorted(near + far)]


def mate(me, k, count):
    found, bit = me, 1
    while bit < count:
        if k & bit:
            found = found + bit * (1 - 2 * lax.rem(lax.div(me, bit), 2))
        bit *= 2
    return found


def greet(me, tp, ep_count, tp_count):
    pairs = tp_count // 2
    pair, side = tp // 2, tp % 2
    barrier = pltpu.get_barrier_semaphore()
    for k in range(1, ep_count):
        pl.semaphore_signal(
            barrier,
            inc=1,
            device_id={"ep": lax.rem(me + k, ep_count), "tp": tp},
            device_id_type=MESH,
        )
    for j in range(1, pairs):
        pl.semaphore_signal(
            barrier,
            inc=1,
            device_id={"ep": me, "tp": lax.rem(pair + j, pairs) * 2 + side},
            device_id_type=MESH,
        )
    pl.semaphore_signal(
        barrier, inc=1, device_id={"ep": me, "tp": pair * 2 + 1 - side}, device_id_type=MESH
    )


def product(left, right, left_axis, right_axis):
    return lax.dot_general(
        left,
        right,
        (((left_axis,), (right_axis,)), ((), ())),
        preferred_element_type=wide,
    )


def iota(shape, axis):
    return lax.broadcasted_iota(jnp.int32, shape, axis)


def thirds(array):
    high = array.astype(kind)
    rest = array - high.astype(wide)
    middle = rest.astype(kind)
    return [high, middle, (rest - middle.astype(wide)).astype(kind)]


def kernel(
    ep_count,
    tp_count,
    pending,
    query_ref,
    forget_ref,
    value_ref,
    opening_ref,
    margin_ref,
    surge_ref,
    head_gain_ref,
    tokens_ref,
    gain_ref,
    routes_ref,
    logits_ref,
    gate_hbm,
    up_hbm,
    down_hbm,
    matrix_hbm,
    mixed_ref,
    moe_ref,
    slots,
    piece,
    both,
    turned,
    down,
    matrix,
    weights,
    note,
    notes,
    guest_weights,
    lifted_ref,
    local_ref,
    window,
    window_total,
    before,
    before_total,
    outgoing,
    incoming,
    parts,
    mix,
    cbuf,
    cmix,
    ysend,
    ysmix,
    ybuf,
    ymix,
    abuf,
    returned,
    guest_abuf,
    guest_returned,
    crossing,
    crossed,
    load,
    sa,
    ra,
    sy,
    ry,
    sc,
    rc,
    ss,
    rs,
    sb,
    rb,
    sz,
    rz,
    sh,
    rh,
    sg,
    rg,
    sn,
    rn,
    su,
    ru,
):
    me, tp = lax.axis_index("ep"), lax.axis_index("tp")
    pairs = tp_count // 2
    pair, side = tp // 2, tp % 2
    other = pair * 2 + 1 - side
    order = visiting_order(ep_count)
    heads, seq_len = surge_ref.shape
    key_width = query_ref.shape[1] // heads
    value_width = value_ref.shape[1] // heads
    tok_rows, width = tokens_ref.shape
    capacity = slots.shape[1]
    units = gate_hbm.shape[0]
    offset = both.shape[0] // 2
    mix_rows = mix.shape[1]
    steps = outgoing.shape[0]
    cuts = (0, ep_count // 2, ep_count * 7 // 8, ep_count)
    first, second, third = [list(range(*cuts[n : n + 2])) for n in range(3)]
    extra = ep_count
    near = [i for i in range(ep_count) if 2 * order[i] < ep_count]
    distant = [i for i in range(ep_count) if i not in near]
    whole_tiles = capacity % 16 == 0
    stride = min(width, 1024) if whole_tiles else width

    fetch = [
        pltpu.make_async_copy(gate_hbm, both.at[pl.ds(0, units)], load.at[0]),
        pltpu.make_async_copy(up_hbm, both.at[pl.ds(offset, units)], load.at[1]),
        pltpu.make_async_copy(down_hbm, down, load.at[2]),
        pltpu.make_async_copy(matrix_hbm, matrix, load.at[3]),
    ]
    for copy in fetch:
        copy.start()

    def remote(src, dst, send, recv, ep, to):
        return pltpu.make_async_remote_copy(
            src_ref=src,
            dst_ref=dst,
            send_sem=send,
            recv_sem=recv,
            device_id={"ep": ep, "tp": to},
            device_id_type=MESH,
        )

    def toward(j):
        return lax.rem(pair + j, pairs)

    def exchange(i):
        to = mate(me, order[i], ep_count)
        return remote(slots.at[i], piece.at[i, tp], sa.at[i], ra.at[i], to, tp)

    def across(i, j):
        to = toward(j) * 2 + side
        return remote(piece.at[i, tp], piece.at[i, tp], sy.at[j, i], ry.at[j, i], me, to)

    def beside(i, j):
        block = lax.rem(pair + pairs - j, pairs) * 2 + side
        return remote(
            piece.at[i, block], piece.at[i, block], sc.at[j, i], rc.at[j, i], me, other
        )

    def back_beside(i, j):
        block = toward(j) * 2 + 1 - side
        if i == extra:
            return remote(mix.at[block], cmix.at[j], sb.at[j, i], rb.at[j, i], me, other)
        return remote(parts.at[i, block], cbuf.at[j, i], sb.at[j, i], rb.at[j, i], me, other)

    def back_across(i, j):
        to = toward(j) * 2 + side
        if i == extra:
            return remote(ysmix.at[j], ymix.at[j], sz.at[j, i], rz.at[j, i], me, to)
        return remote(ysend.at[j, i], ybuf.at[j, i], sz.at[j, i], rz.at[j, i], me, to)

    def home(i):
        to = mate(me, order[i], ep_count)
        return remote(abuf.at[i], returned.at[i], sh.at[i], rh.at[i], to, tp)

    def tell(j):
        return remote(note, notes.at[j], sn.at[j], rn.at[j], me, toward(j) * 2 + side)

    def home_guest(i, j):
        to = mate(me, order[i], ep_count)
        at = near.index(i)
        return remote(
            guest_abuf.at[j, at], guest_returned.at[j, at], sg.at[j, i], rg.at[j, i], to, tp
        )

    def cross(j):
        to = toward(j) * 2 + side
        return remote(crossing.at[j], crossed.at[j], su.at[j], ru.at[j], me, to)

    def back_beside(i, j):
        block = toward(j) * 2 + 1 - side
        if i == extra:
            return remote(mix.at[block], cmix.at[j], sb.at[j, i], rb.at[j, i], me, other)
        return remote(parts.at[i, block], cbuf.at[j, i], sb.at[j, i], rb.at[j, i], me, other)

    def back_across(i, j):
        to = toward(j) * 2 + side
        if i == extra:
            return remote(ysmix.at[j], ymix.at[j], sz.at[j, i], rz.at[j, i], me, to)
        return remote(ysend.at[j, i], ybuf.at[j, i], sz.at[j, i], rz.at[j, i], me, to)

    def home(i):
        to = mate(me, order[i], ep_count)
        return remote(abuf.at[i], returned.at[i], sh.at[i], rh.at[i], to, tp)

    def pass_on(i):
        for j in range(1, pairs):
            across(i, j).start()
        beside(i, 0).start()

    def forward(i):
        exchange(i).wait_recv()
        pass_on(i)

    def relay(i):
        for j in range(1, pairs):
            across(i, j).wait_recv()
            beside(i, j).start()

    rows = tokens_ref[...].astype(wide)
    normed = (
        rows * lax.rsqrt(jnp.mean(rows * rows, axis=-1, keepdims=True) + epsilon) * gain_ref[...]
    ).astype(kind)
    listed = routes_ref[...]
    experts = iota((ep_count, tok_rows), 0)
    strict = (iota((tok_rows, tok_rows), 0) < iota((tok_rows, tok_rows), 1)).astype(kind)

    def spots_of(index):
        routes = listed[:, :tok_rows]
        for t in range(1, tp_count):
            routes = jnp.where(index == t, listed[:, t * tok_rows : (t + 1) * tok_rows], routes)
        named = [routes[i : i + 1, :] for i in range(TOP)]
        tables = [(row == experts).astype(wide) for row in named]
        earlier = product(sum(tables).astype(kind), strict, 1, 0)
        places = [jnp.sum(earlier * table, axis=0, keepdims=True) for table in tables]
        return [row * capacity + place.astype(jnp.int32) for row, place in zip(named, places)]

    places_of = [
        iota((capacity, tok_rows), 0) + mate(me, k, ep_count) * capacity for k in order
    ]

    def choose(spots, tokens, members, store):
        if whole_tiles:
            wanted = jnp.concatenate([places_of[i] for i in members], axis=0)
            chooser = sum((spot == wanted).astype(wide) for spot in spots).astype(kind)
            for c in range(0, width, stride):
                cut = slice(c, c + stride)
                chosen = product(chooser, tokens[:, cut], 1, 0).astype(kind)
                for n, i in enumerate(members):
                    store(i, cut, chosen[n * capacity : (n + 1) * capacity])
        else:
            for i in members:
                chooser = sum((spot == places_of[i]).astype(wide) for spot in spots)
                store(i, slice(None), product(chooser.astype(kind), tokens, 1, 0).astype(kind))

    def keep(i, cut, rows):
        if i:
            slots[i, :, cut] = rows
        else:
            piece[i, tp, :, cut] = rows

    spots = spots_of(tp)
    choose(spots, normed, range(ep_count), keep)
    pl.semaphore_wait(pltpu.get_barrier_semaphore(), ep_count + pairs - 1)
    pass_on(0)
    for i in range(1, ep_count):
        exchange(i).start()

    def share_of(logits):
        raised = jnp.exp(logits - jnp.max(logits, axis=0, keepdims=True))
        return raised / jnp.sum(raised, axis=0, keepdims=True)

    def weigh(spots, share, members, store):
        for i in members:
            weight = sum(
                jnp.where(spot == places_of[i], share[r : r + 1, :], 0.0)
                for r, spot in enumerate(spots)
            )
            high = weight.astype(kind)
            store(i, high, (weight - high.astype(wide)).astype(kind))

    def keep_weight(i, high, low):
        weights[0, i * capacity : (i + 1) * capacity, :] = high
        weights[1, i * capacity : (i + 1) * capacity, :] = low

    note[...] = jnp.zeros_like(note)
    note[:TOP, :tok_rows] = logits_ref[...]
    for j in range(1, pairs):
        tell(j).start()
    weigh(spots, share_of(logits_ref[...]), range(ep_count), keep_weight)
    if units < offset:
        both[units:offset, :] = jnp.zeros((offset - units, width), kind)
        both[offset + units :, :] = jnp.zeros((offset - units, width), kind)

    for copy in pending:
        copy.wait()
    at, since = iota((seq_len, seq_len), 0), iota((seq_len, seq_len), 1)
    shut = jax.nn.sigmoid(-forget_ref[...].astype(wide)) * margin_ref[...]
    within = ((at >= since) & (at // SPAN == since // SPAN)).astype(wide)
    running_all = sum(
        product(within.astype(kind), part, 1, 0) for part in thirds(jnp.log1p(-shut))
    )
    triangle = iota((SPAN, SPAN), 0) >= iota((SPAN, SPAN), 1)

    def recur(head):
        keys = slice(head * key_width, (head + 1) * key_width)
        values = slice(head * value_width, (head + 1) * value_width)
        surges = jnp.sum(within * surge_ref[head : head + 1, :], axis=1, keepdims=True)
        running_head = running_all[:, keys] + surges
        state = jnp.zeros((value_width, key_width), wide)
        total = jnp.zeros((1, key_width), wide)
        for span in range(seq_len // SPAN):
            part = slice(span * SPAN, (span + 1) * SPAN)
            running = running_head[part]
            closing = running[SPAN - 1 : SPAN]
            inflow = shut[part, keys]
            value = value_ref[part, values]
            query = query_ref[part, keys].astype(wide)
            lifted = (query * jnp.exp(running)).astype(kind)
            lowered = (inflow * jnp.exp(-running)).astype(kind)
            scores = jnp.where(triangle, product(lifted, lowered, 1, 1), 0.0)
            local = product(scores.astype(kind), value, 1, 0)
            if span:
                local = local + product(lifted, state.astype(kind), 1, 1)
            local_ref[part, values] = local
            lifted_ref[part, keys] = (query * jnp.exp(running + total)).astype(kind)
            fresh = product(value, (inflow * jnp.exp(closing - running)).astype(kind), 0, 0)
            state = jnp.exp(closing) * state + fresh
            total = total + closing
        window[head] = state
        window_total[head] = total

    def state_copy(step):
        to = lax.rem(me + 2**step, ep_count)
        return remote(outgoing.at[step], incoming.at[step], ss.at[step], rs.at[step], to, tp)

    def send_window(step):
        for head in range(heads):
            outgoing[step, head, :value_width] = window[head].astype(kind)
            total = window_total[head]
            coarse = total.astype(kind).astype(wide)
            line = iota((16, key_width), 0)
            tail = jnp.where(line == 0, coarse, jnp.where(line == 1, total - coarse, 0.0))
            outgoing[step, head, value_width:] = tail.astype(kind)

        @pl.when(me + 2**step < ep_count)
        def _():
            state_copy(step).start()

    def take_window(step):
        @pl.when(me >= 2**step)
        def _():
            state_copy(step).wait_recv()
            for head in range(heads):
                state = incoming[step, head, :value_width].astype(wide)
                total = jnp.sum(
                    incoming[step, head, value_width:].astype(wide), axis=0, keepdims=True
                )
                before[head] = jnp.exp(before_total[head]) * state + before[head]
                before_total[head] = before_total[head] + total
                window[head] = jnp.exp(window_total[head]) * state + window[head]
                window_total[head] = window_total[head] + total

    scanned = []

    def scan():
        if len(scanned) < steps:
            take_window(len(scanned))
            scanned.append(0)
            if len(scanned) < steps:
                send_window(len(scanned))

    def gathered(ref, group, sources=None):
        start, stop = group[0], group[-1] + 1
        if whole_tiles:
            return ref[start:stop].reshape(-1, width)
        if len(ref.shape) == 3:
            return jnp.concatenate([ref[i] for i in group], axis=0)
        return jnp.concatenate([ref[i, t] for i in group for t in range(tp_count)], axis=0)

    def arrive(group):
        for i in group:
            for j in range(pairs):
                beside(i, j).wait_recv()

    def raise_hidden(group):
        result = product(gathered(piece, group), turned[...], 1, 0)
        left, right = result[:, :units], result[:, offset : offset + units]
        return (left * jax.nn.sigmoid(left) * right).astype(kind)

    def lower_hidden(group, hidden):
        start, stop = group[0], group[-1] + 1
        for c in range(0, width, stride):
            cut = slice(c, c + stride)
            result = product(hidden, down[:, cut], 1, 0).astype(kind)
            if whole_tiles:
                parts[start:stop, :, :, cut] = result.reshape(
                    stop - start, tp_count, capacity, stride
                )
            else:
                for n in range((stop - start) * tp_count):
                    i, t = start + n // tp_count, n % tp_count
                    parts[i, t, :, cut] = result[n * capacity : (n + 1) * capacity]

    def leaving(group):
        return sorted(group, key=lambda i: -order[i])

    def hand_over(group):
        for i in group:
            for j in list(range(1, pairs)) + [0]:
                back_beside(i, j).start()

    def fold(i):
        for j in range(1, pairs):
            back_beside(i, j).wait_recv()
            block = toward(j) * 2 + side
            if i == extra:
                ysmix[j] = (mix[block].astype(wide) + cmix[j].astype(wide)).astype(kind)
            else:
                ysend[j, i] = (parts[i, block].astype(wide) + cbuf[j, i].astype(wide)).astype(
                    kind
                )
            back_across(i, j).start()

    def settle(i):
        back_beside(i, 0).wait_recv()
        if i == extra:
            total = mix[tp].astype(wide) + cmix[0].astype(wide)
        else:
            total = parts[i, tp].astype(wide) + cbuf[0, i].astype(wide)
        for j in range(1, pairs):
            back_across(i, j).wait_recv()
            total = total + (ymix[j] if i == extra else ybuf[j, i]).astype(wide)
        if i == extra:
            mixed_ref[...] = total.astype(kind)
        else:
            abuf[i] = total.astype(kind)
            home(i).start()

    def settle_near(i):
        for j in range(1, pairs):
            back_beside(i, j).wait_recv()
            block = toward(j) * 2 + side
            total = (parts[i, block].astype(wide) + cbuf[j, i].astype(wide)).astype(kind)
            if i == 0:
                guest_returned[j, near.index(0)] = total
            else:
                guest_abuf[j, near.index(i)] = total
                home_guest(i, j).start()
        back_beside(i, 0).wait_recv()
        total = (parts[i, tp].astype(wide) + cbuf[0, i].astype(wide)).astype(kind)
        if i == 0:
            returned[i] = total
        else:
            abuf[i] = total
            home(i).start()

    def combine(ref, group, scale):
        start, stop = group[0] * capacity, (group[-1] + 1) * capacity
        taken = gathered(ref, group)
        return product(scale[0, start:stop], taken, 0, 0) + product(
            scale[1, start:stop], taken, 0, 0
        )

    def expert(group):
        arrive(group)
        lower_hidden(group, raise_hidden(group))
        hand_over(group)

    def advance(group):
        for i in group:
            forward(i)
            relay(i - 1)

    def far(group):
        return [i for i in leaving(group) if i in distant]

    def close(group):
        return [i for i in leaving(group) if i in near]

    def fold_all(group):
        for i in group:
            fold(i)

    def settle_all(group):
        for i in group:
            settle(i)

    def settle_close(group):
        for i in close(group):
            settle_near(i)

    def keep_guest_weight(i, high, low):
        at = near.index(i) * capacity
        guest_weights[0, at : at + capacity, :] = high
        guest_weights[1, at : at + capacity, :] = low

    bands = [slice(n, n + 128) for n in range(0, 2 * offset, 128)]
    third_part = -(-len(bands) // 3)

    def turn(part):
        for band in bands[part * third_part : (part + 1) * third_part]:
            turned[:, band] = both[band, :].T

    recur(0)
    advance(first[1:2])
    for head in range(1, heads):
        recur(head)
    before[...] = jnp.zeros_like(before)
    before_total[...] = jnp.zeros_like(before_total)
    send_window(0)
    for copy in fetch[:2]:
        copy.wait()
    turn(0)
    advance(first[2:3])
    turn(1)
    advance(first[3:])
    turn(2)
    for j in range(1, pairs):
        tell(j).wait_recv()
        weigh(
            spots_of(toward(j) * 2 + side),
            share_of(notes[pairs - j][:TOP, :tok_rows]),
            near,
            keep_guest_weight,
        )
    advance(second[:1])
    arrive(first)
    fetch[2].wait()
    hidden = raise_hidden(first)
    advance(second[1:2])
    lower_hidden(first, hidden)
    hand_over(far(first) + close(first))
    advance(second[2:])
    fold_all(far(first)[-1:])
    settle_close(first)
    scan()
    advance(third)
    fold_all(far(first)[:-1])
    arrive(second)
    hidden = raise_hidden(second)
    lower_hidden(second, hidden)
    hand_over(far(second) + close(second))
    settle_all(far(first)[-1:])
    fold_all(far(second))
    relay(ep_count - 1)
    scan()
    settle_all(far(first)[:-1])
    expert(third)
    settle_close(second)
    fold_all(far(third))
    settle_close(third)
    settle_all(far(second))
    for _ in range(steps):
        scan()
    for head in range(heads):
        keys = slice(head * key_width, (head + 1) * key_width)
        values = slice(head * value_width, (head + 1) * value_width)
        out = local_ref[:, values] + product(
            lifted_ref[:, keys], before[head].astype(kind), 1, 1
        )
        out = out * lax.rsqrt(jnp.mean(out * out, axis=-1, keepdims=True) + epsilon)
        opening = opening_ref[:, values].astype(wide)
        lifted_ref[:, values] = (
            out * head_gain_ref[:, values] * (opening * jax.nn.sigmoid(opening))
        ).astype(kind)
    fetch[3].wait()
    for c in range(0, width, stride):
        cut = slice(c, c + stride)
        result = product(lifted_ref[...], matrix[:, cut], 1, 0).astype(kind)
        mix[:, :, cut] = result.reshape(tp_count, mix_rows, stride)
    hand_over([extra])
    fold(extra)
    for j in range(1, pairs):
        for i in near:
            if i:
                home_guest(i, j).wait_recv()
        crossing[j] = combine(guest_returned.at[j], range(len(near)), guest_weights).astype(kind)
        cross(j).start()
    settle_all(far(third))
    for i in first[1:] + second:
        home(i).wait_recv()
    total = combine(returned, first + second, weights)
    settle(extra)
    for i in third:
        home(i).wait_recv()
    total = total + combine(returned, third, weights)
    for j in range(1, pairs):
        cross(j).wait_recv()
        total = total + crossed[j].astype(wide)
    moe_ref[...] = total.astype(kind)

    for i in range(ep_count):
        if i:
            exchange(i).wait_send()
            home(i).wait_send()
    for j in range(1, pairs):
        tell(j).wait_send()
        cross(j).wait_send()
        for i in near:
            if i:
                home_guest(i, j).wait_send()
        for i in distant + [extra]:
            back_across(i, j).wait_send()
        for i in range(ep_count):
            across(i, j).wait_send()
    for i in range(ep_count + 1):
        for j in range(pairs):
            back_beside(i, j).wait_send()
            if i < ep_count:
                beside(i, j).wait_send()
    for step in range(steps):

        @pl.when(me + 2**step < ep_count)
        def _(step=step):
            state_copy(step).wait_send()


def entry(ep_count, tp_count, count, *refs):
    greet(lax.axis_index("ep"), lax.axis_index("tp"), ep_count, tp_count)
    sources, rest = refs[:count], refs[count:]
    middle, staged, arrived, rest = rest[:6], rest[6 : 6 + count], rest[6 + count], rest[7 + count :]
    copies = [
        pltpu.make_async_copy(source, stage, arrived.at[n])
        for n, (source, stage) in enumerate(zip(sources, staged))
    ]
    for copy in copies[7:] + copies[:7]:
        copy.start()
    for copy in copies[7:]:
        copy.wait()
    kernel(ep_count, tp_count, copies[:7], *staged, *middle, *rest)


def run(small, large, heads, capacity, ep_count, tp_count):
    pairs = tp_count // 2
    dma = pltpu.SemaphoreType.DMA
    vmem = pl.BlockSpec(memory_space=pltpu.VMEM)
    hbm = pl.BlockSpec(memory_space=pl.ANY)
    far = pl.BlockSpec(memory_space=pltpu.HBM)
    query, value, tokens = small[0], small[2], small[7]
    gate, _, down, matrix = large
    seq_len, keys = query.shape
    values = value.shape[1]
    tok_rows, width = tokens.shape
    units = gate.shape[0]
    padded = -(-units // 128) * 128
    key_width, value_width = keys // heads, values // heads
    steps = (ep_count - 1).bit_length()
    mix_rows = seq_len // tp_count
    chunks = (ep_count, capacity, width)
    many = (pairs, ep_count + 1)
    nearby = (ep_count // 2, capacity, width)
    state = (steps, heads, value_width + 16, key_width)
    return pl.pallas_call(
        functools.partial(entry, ep_count, tp_count, len(small)),
        out_shape=(
            jax.ShapeDtypeStruct((mix_rows, width), kind),
            jax.ShapeDtypeStruct((tok_rows, width), kind),
        ),
        in_specs=[far] * len(small) + [hbm] * len(large),
        out_specs=(vmem, vmem),
        scratch_shapes=[pltpu.VMEM(part.shape, part.dtype) for part in small]
        + [
            dma((len(small),)),
            pltpu.VMEM(chunks, kind),
            pltpu.VMEM((ep_count, tp_count, capacity, width), kind),
            pltpu.VMEM((2 * padded, width), kind),
            pltpu.VMEM((width, 2 * padded), kind),
            pltpu.VMEM(down.shape, kind),
            pltpu.VMEM(matrix.shape, kind),
            pltpu.VMEM((2, ep_count * capacity, tok_rows), kind),
            pltpu.VMEM((8, 128), wide),
            pltpu.VMEM((pairs, 8, 128), wide),
            pltpu.VMEM((2, nearby[0] * capacity, tok_rows), kind),
            pltpu.VMEM((seq_len, keys), kind),
            pltpu.VMEM((seq_len, values), wide),
            pltpu.VMEM((heads, value_width, key_width), wide),
            pltpu.VMEM((heads, 1, key_width), wide),
            pltpu.VMEM((heads, value_width, key_width), wide),
            pltpu.VMEM((heads, 1, key_width), wide),
            pltpu.VMEM(state, kind),
            pltpu.VMEM(state, kind),
            pltpu.VMEM((ep_count, tp_count, capacity, width), kind),
            pltpu.VMEM((tp_count, mix_rows, width), kind),
            pltpu.VMEM((pairs,) + chunks, kind),
            pltpu.VMEM((pairs, mix_rows, width), kind),
            pltpu.VMEM((pairs,) + chunks, kind),
            pltpu.VMEM((pairs, mix_rows, width), kind),
            pltpu.VMEM((pairs,) + chunks, kind),
            pltpu.VMEM((pairs, mix_rows, width), kind),
            pltpu.VMEM(chunks, kind),
            pltpu.VMEM(chunks, kind),
            pltpu.VMEM((pairs,) + nearby, kind),
            pltpu.VMEM((pairs,) + nearby, kind),
            pltpu.VMEM((pairs, tok_rows, width), kind),
            pltpu.VMEM((pairs, tok_rows, width), kind),
            dma((4,)),
            dma((ep_count,)),
            dma((ep_count,)),
            dma(many),
            dma(many),
            dma(many),
            dma(many),
            dma((steps,)),
            dma((steps,)),
            dma(many),
            dma(many),
            dma(many),
            dma(many),
            dma((ep_count,)),
            dma((ep_count,)),
            dma(many),
            dma(many),
            dma((pairs,)),
            dma((pairs,)),
            dma((pairs,)),
            dma((pairs,)),
        ],
        compiler_params=pltpu.CompilerParams(
            collective_id=0, has_side_effects=True, vmem_limit_bytes=60 << 20
        ),
    )(*small, *large)


def hand_out_kernel(mixed_in, moe_in, mixed_out, moe_out):
    mixed_out[...] = mixed_in[...]
    moe_out[...] = moe_in[...]


def hand_out(mixed, moe):
    vmem = pl.BlockSpec(memory_space=pltpu.VMEM)
    return pl.pallas_call(
        hand_out_kernel,
        out_shape=tuple(jax.ShapeDtypeStruct(part.shape, part.dtype) for part in (mixed, moe)),
        in_specs=[vmem] * 2,
        out_specs=(vmem, vmem),
    )(mixed, moe)


def per_device(
    recurrence_query,
    forget_preactivation,
    recurrence_value,
    output_gate_preactivation,
    forget_margin,
    surge_log_decay,
    head_norm_gain,
    recurrence_output_matrix,
    second_micro_input,
    expert_norm_gain,
    routes,
    router_chosen_logits,
    expert_gate_matrix,
    expert_up_matrix,
    expert_down_matrix,
):
    tp_count = lax.axis_size("tp")
    expert_count = lax.axis_size("ep")
    tok_rows = second_micro_input.shape[0]
    capacity = 2 * tok_rows * TOP // expert_count
    small = (
        recurrence_query,
        forget_preactivation,
        recurrence_value,
        output_gate_preactivation,
        forget_margin[None, :],
        surge_log_decay,
        head_norm_gain[None, :],
        second_micro_input,
        expert_norm_gain[None, :],
        routes.T,
        router_chosen_logits.T,
    )
    large = (
        expert_gate_matrix[0].T,
        expert_up_matrix[0].T,
        expert_down_matrix[0],
        recurrence_output_matrix,
    )
    heads = surge_log_decay.shape[0]
    return hand_out(*run(small, large, heads, capacity, expert_count, tp_count))


def solution(mesh):
    return jax.shard_map(
        per_device,
        mesh=mesh,
        in_specs=(
            P("ep", "tp"),
            P("ep", "tp"),
            P("ep", "tp"),
            P("ep", "tp"),
            P("tp"),
            P("tp", "ep"),
            P("tp"),
            P("tp", None),
            P(("ep", "tp"), None),
            P(),
            P("ep", None),
            P(("ep", "tp"), None),
            P("ep", None, "tp"),
            P("ep", None, "tp"),
            P("ep", "tp", None),
        ),
        out_specs=(P(("ep", "tp"), None), P(("ep", "tp"), None)),
        check_vma=False,
    )
```
